32 devices in a mesh: sp: 8 (over z, x), tp: 4 (over y, core).
Axes of the slice: x: 2, y: 2, z: 4, core: 2. Of those that a mesh axis runs over, the one named last changes fastest.
Arguments:
- residual: bfloat16 [2048, 2048], P(('sp', 'tp')), may hold values from -6 to 6
- first_query: bfloat16 [2048, 512], P('sp', 'tp'), may hold values from -6 to 6
- second_query: bfloat16 [2048, 512], P('sp', 'tp'), may hold values from -6 to 6
- first_key: bfloat16 [2048, 512], P('sp', 'tp'), may hold values from -6 to 6
- second_key: bfloat16 [2048, 512], P('sp', 'tp'), may hold values from -6 to 6
- values: bfloat16 [2048, 1024], P('sp', 'tp'), may hold values from -6 to 6
- lambdas: float32 [8], P('tp'), may hold values from 0.3 to 0.8
- head_gain: float32 [128], replicated, may hold values from 0.1 to 1.9
- out_weight: bfloat16 [1024, 2048], P('tp'), may hold values from -0.1875 to 0.1875
- norm_gain: float32 [2048], replicated, may hold values from 0.1 to 1.9
- up_weight: bfloat16 [2048, 4096], P('sp', 'tp'), may hold values from -0.125 to 0.125
- down_weight: bfloat16 [4096, 2048], P('tp', 'sp'), may hold values from -0.09375 to 0.09375
Outputs:
- mixed: bfloat16 [2048, 2048], P(('sp', 'tp'))
The draws below stay inside these ranges and needn't reach their ends.
All inputs are finite; a program needn't handle non-finite values.
Results may differ from the reference program's by a relative error of at most 0.019.
Values may be sent and summed in bfloat16 or wider, within the bound.
A program may use at most 128 MiB of HBM per device.

```python
import jax
import jax.numpy as jnp
from jax import lax

D = 2048
HEADS = 8
HEAD = 64
VDIM = 128
FF = 4096
TOK_DEV = 256
TOKENS = 2048


def draw_entries(key, which_map, which_role):
    own_key = jax.random.fold_in(key, 100 * which_map + which_role)
    width = HEADS * HEAD
    data = jnp.clip(1.3 * jax.random.normal(own_key, (TOKENS, width), jnp.float32), -6.0, 6.0)
    return data.astype(jnp.bfloat16)


def draw_first_query(key, part):
    return draw_entries(key, 1, 0)


def draw_first_key(key, part):
    return draw_entries(key, 1, 1)


def draw_second_query(key, part):
    return draw_entries(key, 2, 0)


def draw_second_key(key, part):
    return draw_entries(key, 2, 1)


def steps_of(key, shape, split, least, top_value):
    level, own = 1.0, jax.random.fold_in(key, 6)
    for axis_at, blocks in split:
        heights = jnp.exp(jax.random.uniform(jax.random.fold_in(own, axis_at), (blocks,), jnp.float32, least / len(split), top_value / len(split)))
        level = level * jnp.repeat(heights, shape[axis_at] // blocks).reshape([-1 if axis == axis_at else 1 for axis in range(len(shape))])
    return level


def gaussian(key, dims, scale, most, shards=(), held_as=jnp.bfloat16):
    result = jax.random.normal(key, dims, jnp.float32) * scale
    if len(shards) > 0:
        result = steps_of(key, dims, shards, -0.22, 0.18) * result
    return jnp.clip(result, min=-most, max=most).astype(held_as)


def setup_inputs(seed: int = 0) -> dict:
    arg_keys = jax.random.split(jax.random.key(seed), 13)
    residual = gaussian(arg_keys[0], (TOKENS, D), 1.0, 6.0, ((0, 32),))
    first_query = draw_first_query(jax.random.fold_in(arg_keys[12], 71), 0)
    second_query = draw_second_query(jax.random.fold_in(arg_keys[12], 71), 0)
    first_key = draw_first_key(jax.random.fold_in(arg_keys[12], 71), 0)
    second_key = draw_second_key(jax.random.fold_in(arg_keys[12], 71), 0)
    values = gaussian(arg_keys[5], (TOKENS, HEADS * VDIM), 1.0, 6.0, ((0, 8), (1, 4)))
    lambdas = jnp.clip(0.3 + 0.5 * jax.random.uniform(arg_keys[6], (HEADS,), jnp.float32) ** steps_of(arg_keys[6], (HEADS,), ((0, 4),), -0.2, 0.2), 0.3, 0.8)
    head_gain = jnp.clip(1.0 + 0.18 * jax.random.normal(arg_keys[7], (VDIM,), jnp.float32), 0.1, 1.9)
    out_weight = gaussian(arg_keys[8], (HEADS * VDIM, D), (HEADS * VDIM) ** -0.5, 0.1875, ((0, 4),))
    norm_gain = jnp.clip(1.0 + 0.18 * jax.random.normal(arg_keys[9], (D,), jnp.float32), 0.1, 1.9)
    up_weight = gaussian(arg_keys[10], (D, FF), D ** -0.5, 0.125, ((0, 8), (1, 4)))
    down_weight = gaussian(arg_keys[11], (FF, D), FF ** -0.5, 0.09375, ((0, 4), (1, 8)))
    return dict(residual=residual, first_query=first_query, second_query=second_query, first_key=first_key, second_key=second_key, values=values, lambdas=lambdas, head_gain=head_gain, out_weight=out_weight, norm_gain=norm_gain, up_weight=up_weight, down_weight=down_weight)


def rotate(blocked, positions):
    half = blocked.shape[-1] // 2
    inverse = 10000.0 ** (-jnp.arange(0, half, dtype=jnp.float32) * 2.0 / blocked.shape[-1])
    angle = positions[:, None] * inverse[None, :]
    cosine = jnp.cos(angle)[:, None, :]
    sine = jnp.sin(angle)[:, None, :]
    first, second = (blocked[..., :half], blocked[..., half:])
    return jnp.concatenate([first * cosine - second * sine, second * cosine + first * sine], axis=-1)

def attend(queries, keys, vals):
    scores = jnp.dot(queries, keys.T, preferred_element_type=jnp.float32) * HEAD ** (-0.5)
    peak = lax.optimization_barrier(jnp.max(scores, axis=-1, keepdims=True))
    weights = jnp.exp(scores - peak)
    total = lax.optimization_barrier(jnp.sum(weights, axis=-1, keepdims=True))
    summed = jnp.dot(weights.astype(jnp.bfloat16), vals, preferred_element_type=jnp.float32)
    return summed / total

def layer_norm(stream, gain):
    center = stream - lax.optimization_barrier(jnp.mean(stream, axis=-1, keepdims=True))
    spread = lax.optimization_barrier(jnp.mean(center * center, axis=-1, keepdims=True))
    return center * lax.rsqrt(spread + 1e-05) * gain

def reference(residual, first_query, second_query, first_key, second_key, values, lambdas, head_gain, out_weight, norm_gain, up_weight, down_weight):
    length = residual.shape[0]
    positions = jnp.arange(length, dtype=jnp.float32)

    def prepare(source):
        turned = rotate(source.astype(jnp.float32).reshape(length, HEADS, HEAD), positions)
        return turned.astype(jnp.bfloat16).transpose(1, 0, 2)
    query_a, query_b = (prepare(first_query), prepare(second_query))
    key_a, key_b = (prepare(first_key), prepare(second_key))
    vals = values.reshape(length, HEADS, VDIM).transpose(1, 0, 2)

    def one_head(item):
        part_a, part_b, keys_a, keys_b, head_vals, weight = item

        def one_block(pair):
            return attend(pair[0], keys_a, head_vals) - weight * attend(pair[1], keys_b, head_vals)
        blocks = lax.map(one_block, (part_a.reshape(-1, TOK_DEV, HEAD), part_b.reshape(-1, TOK_DEV, HEAD)))
        return blocks.reshape(length, VDIM)
    diff = lax.map(one_head, (query_a, query_b, key_a, key_b, vals, lambdas))
    scale = lax.rsqrt(lax.optimization_barrier(jnp.mean(diff * diff, axis=-1, keepdims=True)) + 1e-05)
    heads_out = (diff * scale * head_gain * 0.8).astype(jnp.bfloat16)
    flat = heads_out.transpose(1, 0, 2).reshape(length, HEADS * VDIM)
    projected = jnp.dot(flat, out_weight, preferred_element_type=jnp.float32)
    normed = layer_norm(residual.astype(jnp.float32) + projected, norm_gain).astype(jnp.bfloat16)
    lifted = jnp.dot(normed, up_weight, preferred_element_type=jnp.float32)
    hidden = jnp.square(jax.nn.relu(lifted)).astype(jnp.bfloat16)
    lowered = jnp.dot(hidden, down_weight, preferred_element_type=jnp.float32)
    return (normed.astype(jnp.float32) + lowered).astype(jnp.bfloat16)
```

```python
import functools

import jax
import jax.numpy as jnp
import numpy as np
from jax import lax
from jax.experimental import pallas as pl
from jax.experimental.pallas import tpu as pltpu
from jax.sharding import PartitionSpec as P


def rotate(blocked, positions):
    half = blocked.shape[-1] // 2
    inverse = 10000.0 ** (-jnp.arange(0, half, dtype=jnp.float32) * 2.0 / blocked.shape[-1])
    angle = positions[:, None] * inverse[None, :]
    cosine = jnp.cos(angle)[:, None, :]
    sine = jnp.sin(angle)[:, None, :]
    first, second = (blocked[..., :half], blocked[..., half:])
    return jnp.concatenate(
        [first * cosine - second * sine, second * cosine + first * sine], axis=-1
    )


def absorb(state, queries, keys, vals, factor):
    top, total, summed = state
    scores = jnp.einsum("qhe,khe->qhk", queries, keys, preferred_element_type=jnp.float32) * factor
    peak = jnp.maximum(top, jnp.max(scores, axis=-1))
    shrink = jnp.exp(top - peak)
    weights = jnp.exp(scores - peak[..., None])
    total = total * shrink + jnp.sum(weights, axis=-1)
    summed = summed * shrink[..., None] + jnp.einsum(
        "qhk,khe->qhe", weights.astype(jnp.bfloat16), vals, preferred_element_type=jnp.float32
    )
    return (peak, total, summed)


def layer_norm(stream, gain):
    center = stream - jnp.mean(stream, axis=-1, keepdims=True)
    spread = jnp.mean(center * center, axis=-1, keepdims=True)
    return center * lax.rsqrt(spread + 1e-05) * gain


def local(
    residual,
    first_query,
    second_query,
    first_key,
    second_key,
    values,
    lambdas,
    head_gain,
    out_weight,
    norm_gain,
    up_weight,
    down_weight,
):
    local_rows = first_query.shape[0]
    head_count = lambdas.shape[0]
    head_width = first_query.shape[1] // head_count
    value_width = values.shape[1] // head_count
    quarter_rows = local_rows // lax.axis_size("tp")
    factor = head_width ** (-0.5)
    positions = (lax.axis_index("sp") * local_rows + jnp.arange(local_rows)).astype(jnp.float32)

    def prepare(source):
        turned = rotate(
            source.astype(jnp.float32).reshape(local_rows, head_count, head_width), positions
        )
        return turned.astype(jnp.bfloat16)

    query_a, query_b = (prepare(first_query), prepare(second_query))
    key_a = prepare(first_key).reshape(local_rows, head_count * head_width)
    key_b = prepare(second_key).reshape(local_rows, head_count * head_width)
    start_state = (
        jnp.full((local_rows, head_count), -1e30, jnp.float32),
        jnp.zeros((local_rows, head_count), jnp.float32),
        jnp.zeros((local_rows, head_count, value_width), jnp.float32),
    )
    piece_a = lax.all_gather(key_a, "sp", axis=0, tiled=True)
    piece_b = lax.all_gather(key_b, "sp", axis=0, tiled=True)
    piece_v = lax.all_gather(values, "sp", axis=0, tiled=True)
    count = piece_a.shape[0]
    block = 512
    blocks = count // block

    def advance(state, item):
        block_a, block_b, block_v = item
        return (
            (
                absorb(state[0], query_a, block_a, block_v, factor),
                absorb(state[1], query_b, block_b, block_v, factor),
            ),
            None,
        )

    items = (
        piece_a.reshape(blocks, block, head_count, head_width),
        piece_b.reshape(blocks, block, head_count, head_width),
        piece_v.reshape(blocks, block, head_count, value_width),
    )
    state_a, state_b = lax.scan(advance, (start_state, start_state), items)[0]
    diff = state_a[2] / state_a[1][..., None] - lambdas[None, :, None] * (
        state_b[2] / state_b[1][..., None]
    )
    scale = lax.rsqrt(jnp.mean(diff * diff, axis=-1, keepdims=True) + 1e-05)
    flat = (
        (diff * scale * head_gain * 0.8)
        .astype(jnp.bfloat16)
        .reshape(local_rows, head_count * value_width)
    )
    projected = lax.psum(
        jnp.dot(flat, out_weight, preferred_element_type=jnp.float32).astype(jnp.bfloat16), "tp"
    ).astype(jnp.float32)
    stream = lax.all_gather(residual, "tp", axis=0, tiled=True)
    whole = layer_norm(stream.astype(jnp.float32) + projected, norm_gain).astype(jnp.bfloat16)
    own_normed = lax.dynamic_slice_in_dim(
        whole, lax.axis_index("tp") * quarter_rows, quarter_rows, 0
    )
    lifted = jnp.dot(
        whole,
        lax.all_gather(up_weight, "sp", axis=0, tiled=True),
        preferred_element_type=jnp.float32,
    )
    down_full = lax.all_gather(down_weight, "sp", axis=1, tiled=True)
    hidden = jnp.square(jax.nn.relu(lifted)).astype(jnp.bfloat16)
    lowered = lax.psum_scatter(
        jnp.dot(hidden, down_full, preferred_element_type=jnp.float32).astype(jnp.bfloat16),
        "tp",
        scatter_dimension=0,
        tiled=True,
    ).astype(jnp.float32)
    return (own_normed.astype(jnp.float32) + lowered).astype(jnp.bfloat16)


BF = jnp.bfloat16
F32 = jnp.float32
VMEM_BUDGET = 40 * 2**20
PIECES = 2
MESH = pl.DeviceIdType.MESH


def receive_slots(nz):
    sizes = dict(kvz=nz, kvx=nz, kvs=nz, kvt=nz, q=nz, head=2 * nz, lam=1, ow=6, norm=6)
    for name in ("up", "dn"):
        for way in "zxst":
            sizes[name + way] = nz * PIECES
    sizes.update(yg=2 * nz * PIECES, zg=2 * nz * PIECES)
    base, at = {}, 0
    for name, size in sizes.items():
        base[name] = at
        at += size
    return base, at


def layer_kernel(
    nz, head_width,
    qa_far, qb_far, ka_far, kb_far, v_far, inverse, lam, hgain, ow0, res0, ngain, up0, dn0,
    out,
    kvs, qs, kv, qb, qm, lamt, hsrc, hb, up, dn, ow, nb, hidden, mine, part, ygot, zsend, zgot,
    top, total, summed, send, recv, load, qa, qbb, ka, kb,
):
    s = lax.axis_index("sp")
    t = lax.axis_index("tp")
    z, x, y, c = s // 2, s % 2, t // 2, t % 2
    zl = z % 2
    base, _ = receive_slots(nz)
    rows, width = ka.shape
    piece = res0.shape[0]
    depth = up0.shape[0]
    units = up0.shape[1]
    half_rows = rows // 2
    P_ = PIECES

    def dev(x_, y_, z_, c_):
        return {"sp": z_ * 2 + x_, "tp": y_ * 2 + c_}

    sib = dev(x, y, z, 1 - c)
    xnb = dev(1 - x, y, z, c)
    ynb = dev(x, 1 - y, z, c)
    znb = dev(x, y, z + 1 - 2 * zl, c)
    order = [z, z + 1 - 2 * zl, (z + 2) % nz, nz - 1 - z]

    loads = [
        pltpu.make_async_copy(src, dst, load.at[i])
        for i, (src, dst) in enumerate((
            (ka_far, ka), (kb_far, kb), (qa_far, qa), (qb_far, qbb),
            (v_far.at[:, :width], kvs.at[0, :, width:]), (v_far.at[:, width:], kvs.at[1, :, width:]),
            (ow0, ow.at[t]),
        ))
    ]
    for cp in loads:
        cp.start()
    barrier = pltpu.get_barrier_semaphore()
    peers = [xnb, sib]
    peers += [dev(x, y, (z + k) % nz, d) for k in range(1, nz) for d in range(2)]
    peers += [dev(x, 1 - y, (z + k) % nz, c) for k in range(nz)]
    for peer in peers:
        pl.semaphore_signal(barrier, inc=1, device_id=peer, device_id_type=MESH)

    started = []

    def remote(src, dst, slot, peer, unless=None, local=False):
        i = len(started)
        cp = pltpu.make_async_remote_copy(
            src_ref=src, dst_ref=dst, send_sem=send.at[i], recv_sem=recv.at[slot],
            device_id=peer, device_id_type=MESH,
        )
        started.append((cp, unless))
        if unless is None:
            cp.start()
        else:
            pl.when(jnp.logical_not(unless))(cp.start)
            if local:
                pl.when(unless)(pltpu.make_async_copy(src, dst, recv.at[slot]).start)

    def got(dst, slot, unless=None):
        cp = pltpu.make_async_remote_copy(
            src_ref=dst, dst_ref=dst, send_sem=send.at[0], recv_sem=recv.at[slot],
            device_id=sib, device_id_type=MESH,
        )
        if unless is None:
            cp.wait_recv()
        else:
            pl.when(jnp.logical_not(unless))(cp.wait_recv)

    def ow_half(ref, i):
        return ref.at[pl.ds(i * (rows // 2), rows // 2)]

    weights = {"up": (up0, up), "dn": (dn0, dn)}

    def spread(name, far, pieces=range(P_)):
        own, buf = weights[name]
        size = buf.shape[4]
        span = buf.shape[5]
        for p in pieces:
            for z_t in (c, c + 2):
                for d in range(2):
                    if name == "up":
                        src = own.at[pl.ds((d * P_ + p) * size, size)]
                    else:
                        src = own.at[pl.ds(d * size, size), pl.ds(p * span, span)]
                    dst = buf.at[x, z, p, d]
                    slot = base[name + "z"] + z * P_ + p
                    here = z_t == z
                    skip = here if far else jnp.logical_not(here)
                    if far:
                        remote(src, dst, slot, dev(x, y, z_t, d), unless=here)
                    else:
                        i = len(started)
                        cp = pltpu.make_async_remote_copy(
                            src_ref=src, dst_ref=dst, send_sem=send.at[i], recv_sem=recv.at[slot],
                            device_id=sib, device_id_type=MESH,
                        )
                        away = jnp.logical_or(skip, d == c)
                        started.append((cp, away))
                        pl.when(jnp.logical_not(away))(cp.start)
                        near = jnp.logical_and(here, d == c)
                        pl.when(near)(pltpu.make_async_copy(src, dst, recv.at[slot]).start)

    def relay_z(name, k, pieces=range(P_)):
        buf = weights[name][1]
        zz = order[k]
        for p in pieces:
            ref = buf.at[x, zz, p, c]
            got(ref, base[name + "z"] + zz * P_ + p)
            remote(ref, ref, base[name + "x"] + zz * P_ + p, xnb)
            remote(ref, ref, base[name + "s"] + zz * P_ + p, sib)

    def relay_x(name, k, pieces=range(P_)):
        buf = weights[name][1]
        zz = order[k]
        for p in pieces:
            ref = buf.at[1 - x, zz, p, c]
            got(ref, base[name + "x"] + zz * P_ + p)
            remote(ref, ref, base[name + "t"] + zz * P_ + p, sib)

    def settle(name, k, other, pieces=range(P_)):
        buf = weights[name][1]
        zz = order[k]
        for p in pieces:
            ref = buf.at[1 - x if other else x, zz, p, 1 - c]
            got(ref, base[name + ("t" if other else "s")] + zz * P_ + p)

    half = head_width // 2
    lane = lax.broadcasted_iota(jnp.int32, (rows, width), 1)
    low = (lane % head_width) < half
    front = lane < head_width
    position = (lax.broadcasted_iota(jnp.int32, (rows, width), 0) + s * rows).astype(F32)
    angle = position * inverse[...]
    cos = jnp.cos(angle)
    sin = jnp.sin(angle)
    sin = jnp.where(low, -sin, sin)

    def turn(ref):
        v = ref[...].astype(F32)
        other = jnp.where(low, pltpu.roll(v, width - half, 1), pltpu.roll(v, half, 1))
        return v * cos + other * sin

    def packed(a, b):
        first = jnp.where(front, a, pltpu.roll(b, head_width, 1))
        second = jnp.where(front, pltpu.roll(a, head_width, 1), b)
        return first.astype(BF), second.astype(BF)

    lamt[0] = jnp.full(lamt.shape[1:], lam[zl], F32)
    pl.semaphore_wait(barrier, len(peers))
    spread("up", False)
    for i in range(2):
        remote(ow_half(ow0, i), ow_half(ow.at[t], i), base["ow"] + 2 + i, ynb)
    for i in range(2):
        remote(ow_half(ow0, i), ow_half(ow.at[t], i), base["ow"] + i, sib)
    for cp in loads[:2]:
        cp.wait()
    for j, v in enumerate(packed(turn(ka), turn(kb))):
        kvs[j, :, :width] = v
    for cp in loads[4:6]:
        cp.wait()
    for j in range(2):
        z_t = 2 * c + j
        for d in range(2):
            remote(
                kvs.at[j, pl.ds(d * half_rows, half_rows)], kv.at[x, z, d], base["kvz"] + z,
                dev(x, y, z_t, d), unless=jnp.logical_and(z_t == z, d == c),
            )
    for cp in loads[2:4]:
        cp.wait()
    scale = head_width ** (-0.5)
    for j, v in enumerate(packed(turn(qa), turn(qbb))):
        qs[j] = (v.astype(F32) * scale).astype(BF).reshape(qs.shape[1:])
    for j in range(2):
        z_t = 2 * c + j
        for d in range(2):
            remote(
                qs.at[j, :, d], qb.at[z], base["q"] + z,
                dev(x, y, z_t, d), unless=jnp.logical_and(z_t == z, d == c),
            )
    remote(lamt.at[0], lamt.at[1], base["lam"], sib)
    mine_here = c == z // 2

    @pl.when(mine_here)
    def _():
        kv[x, z, c] = kvs[zl, pl.ds(pl.multiple_of(c * half_rows, half_rows), half_rows), :]
        for i in range(2):
            qb[z, i] = qs[zl, i, c]

    spread("up", True, [0])
    relay_z("up", 0)

    def relay_kv(k):
        zz = order[k]
        ref = kv.at[x, zz, c]
        got(ref, base["kvz"] + zz, mine_here if k == 0 else None)
        remote(ref, ref, base["kvx"] + zz, xnb)
        remote(ref, ref, base["kvs"] + zz, sib)

    for k in range(nz):
        relay_kv(k)
    for k in range(nz):
        got(qb.at[order[k]], base["q"] + order[k], mine_here if k == 0 else None)
    spread("dn", False)
    queries = qb[...].reshape(-1, width)
    first_lanes = lax.broadcasted_iota(jnp.int32, queries.shape, 1) < head_width
    zero = jnp.zeros_like(queries)
    qm[0] = jnp.where(first_lanes, queries, zero)
    qm[1] = jnp.where(first_lanes, zero, queries)
    tiles = top.shape[1]
    tile = queries.shape[0] // tiles

    def attend(xi, first):
        def body(qt, carry):
            block = kv[xi].reshape(-1, 2 * width)
            keys = block[:, :width]
            vals = block[:, width:]
            at = pl.ds(pl.multiple_of(qt * tile, tile), tile)
            for m in range(2):
                scores = lax.dot_general(
                    keys, qm[m, at, :], (((1,), (1,)), ((), ())), preferred_element_type=F32
                )
                peak = jnp.max(scores, axis=0, keepdims=True)
                if not first:
                    old = top[m, qt]
                    peak = jnp.maximum(old, peak)
                    shrink = jnp.exp(old - peak)
                e = jnp.exp(scores - peak)
                row = jnp.sum(e, axis=0, keepdims=True)
                acc = lax.dot_general(
                    vals, e.astype(BF), (((0,), (0,)), ((), ())), preferred_element_type=F32
                )
                if first:
                    top[m, qt] = peak
                else:
                    row += total[m, qt] * shrink
                    acc += summed[m, qt] * shrink
                total[m, qt] = row
                summed[m, qt] = acc
            return carry

        lax.fori_loop(0, tiles, body, 0)

    for k in range(nz):
        zz = order[k]
        got(kv.at[x, zz, 1 - c], base["kvs"] + zz)
    relay_z("dn", 0)
    attend(x, True)
    for k in range(nz):
        zz = order[k]
        ref = kv.at[1 - x, zz, c]
        got(ref, base["kvx"] + zz)
        remote(ref, ref, base["kvt"] + zz, sib)
    relay_x("up", 0)
    spread("up", True, [1])
    for k in range(nz):
        zz = order[k]
        got(kv.at[1 - x, zz, 1 - c], base["kvt"] + zz)
    attend(1 - x, False)

    there = 2 * (1 - y) + c
    got(lamt.at[1], base["lam"])
    weight = jnp.where(mine_here, lamt[0], lamt[1])[:1, :1]
    per = nz // tiles
    me = y * nz + z
    for qt in range(tiles):
        a = summed[0, qt] / total[0, qt]
        b = summed[1, qt] / total[1, qt]
        diff = a - weight * b
        norm = lax.rsqrt(jnp.mean(diff * diff, axis=0, keepdims=True) + 1e-05)
        done = ((diff * norm).T * hgain[...] * 0.8).astype(BF)
        hsrc[qt * per : (qt + 1) * per] = done.reshape((per,) + hsrc.shape[1:])
        for z_t in range(qt * per, (qt + 1) * per):
            for y_t in range(2):
                remote(
                    hsrc.at[z_t, y_t], hb.at[me], base["head"] + me, dev(x, y_t, z_t, c),
                    unless=jnp.logical_and(z == z_t, y == y_t),
                )
    hb[me] = hsrc[z, y]
    for k in range(1, nz):
        relay_z("up", k, [0])
    for i in range(2):
        got(ow_half(ow.at[there], i), base["ow"] + 2 + i)
        remote(ow_half(ow.at[there], i), ow_half(ow.at[there], i), base["ow"] + 4 + i, sib)
    for other in range(1, 2 * nz):
        k, dy = other % nz, other // nz
        src = ((y + dy) % 2) * nz + (z + k) % nz
        got(hb.at[src], base["head"] + src)
    loads[6].wait()
    for i in range(2):
        got(ow_half(ow.at[t + 1 - 2 * c], i), base["ow"] + i)
        got(ow_half(ow.at[there + 1 - 2 * c], i), base["ow"] + 4 + i)

    stream = res0[...].astype(F32)
    for tt in range(ow.shape[0]):
        pair = jnp.concatenate([hb[2 * tt], hb[2 * tt + 1]], axis=-1)
        stream += jnp.dot(pair, ow[tt], preferred_element_type=F32)
    center = stream - jnp.mean(stream, axis=-1, keepdims=True)
    spread_ = jnp.mean(center * center, axis=-1, keepdims=True)
    own = 2 * y + zl
    nb[own] = (center * lax.rsqrt(spread_ + 1e-05) * ngain[...]).astype(BF)
    zn = 2 * y + 1 - zl
    def nb_half(m, i):
        return nb.at[m, pl.ds(i * (piece // 2), piece // 2)]

    for i in range(2):
        remote(nb_half(own, i), nb_half(own, i), base["norm"] + i, znb)
        remote(nb_half(own, i), nb_half(own, i), base["norm"] + 2 + i, ynb)
    spread("dn", True, [0])
    for k in range(1, nz):
        relay_x("up", k, [0])
    for i in range(2):
        got(nb_half(zn, i), base["norm"] + i)
        remote(nb_half(zn, i), nb_half(zn, i), base["norm"] + 4 + i, ynb)
    for k in range(1, nz):
        relay_z("up", k, [1])
    spread("dn", True, [1])
    relay_x("dn", 0)
    for k in range(1, nz):
        relay_x("up", k, [1])
    for i in range(2):
        got(nb_half(2 * (1 - y) + zl, i), base["norm"] + 2 + i)
        got(nb_half(2 * (1 - y) + 1 - zl, i), base["norm"] + 4 + i)
    for k in range(nz):
        settle("up", k, False)
        settle("up", k, True)
    normed = nb[...].reshape(-1, nb.shape[2])
    lifted = None
    for zz in range(nz):
        for xx in range(2):
            at = (2 * zz + xx) * depth
            block = jnp.concatenate([up[xx, zz, p, d] for d in range(2) for p in range(P_)], axis=0)
            term = jnp.dot(normed[:, at : at + depth], block, preferred_element_type=F32)
            lifted = term if lifted is None else lifted + term
    lifted = jnp.maximum(lifted, 0.0)
    hidden[...] = (lifted * lifted).astype(BF)

    def lower(k, other, p):
        zz, xx = order[k], (1 - x if other else x)
        settle("dn", k, other, [p])
        i = (2 * zz + xx) * P_ + p
        r = jnp.dot(hidden[...], dn[xx, zz, p].reshape(units, -1), preferred_element_type=F32)
        r = r.reshape(mine.shape[1:])
        mine[i] = r
        part[i] = r.astype(BF)
        remote(part.at[i, pl.ds(2 * (1 - y), 2)], ygot.at[i], base["yg"] + i, ynb)
        return i

    def middle(i):
        got(ygot.at[i], base["yg"] + i)
        zsend[i] = (mine[i, zn] + ygot[i, 1 - zl].astype(F32)).astype(BF)
        remote(zsend.at[i], zgot.at[i], base["zg"] + i, znb)

    def finish(i):
        got(zgot.at[i], base["zg"] + i)
        span = mine.shape[3]
        at = pl.ds(pl.multiple_of(i * span, span), span)
        r = nb[own, :, at].astype(F32) + mine[i, own] + ygot[i, zl].astype(F32) + zgot[i].astype(F32)
        out[:, at] = r.astype(BF)

    done = []
    mid_at = 0
    for p in range(P_):
        for k in range(1, nz):
            relay_z("dn", k, [p])
        for k in range(nz):
            if k:
                relay_x("dn", k, [p])
            for other in (False, True):
                done.append(lower(k, other, p))
                if len(done) - mid_at > 2:
                    middle(done[mid_at])
                    mid_at += 1
    while mid_at < len(done):
        middle(done[mid_at])
        mid_at += 1
    for i in done:
        finish(i)
    for cp, unless in started:
        if unless is None:
            cp.wait_send()
        else:
            pl.when(jnp.logical_not(unless))(cp.wait_send)


def fused(n, nt, residual, first_query, second_query, first_key, second_key, values,
          lambdas, head_gain, out_weight, norm_gain, up_weight, down_weight):
    rows, width = first_query.shape
    heads = lambdas.shape[0]
    head_width = width // heads
    value_width = values.shape[1] // heads
    half = head_width // 2
    depth, units = up_weight.shape
    model = out_weight.shape[1]
    piece = residual.shape[0]
    nz = n // 2
    inverse = 10000.0 ** (-np.arange(half) * 2.0 / head_width)
    inverse = np.tile(inverse, 2 * heads)[None, :].astype(np.float32)
    vmem = pl.BlockSpec(memory_space=pltpu.VMEM)
    smem = pl.BlockSpec(memory_space=pltpu.SMEM)
    far = pl.BlockSpec(memory_space=pl.ANY)
    queries = rows * 2
    tiles = 2
    _, slots = receive_slots(nz)
    return pl.pallas_call(
        functools.partial(layer_kernel, nz, head_width),
        out_shape=jax.ShapeDtypeStruct((piece, model), BF),
        in_specs=[far] * 5 + [vmem, smem, vmem, far, vmem, vmem, far, far],
        out_specs=vmem,
        scratch_shapes=[
            pltpu.VMEM((2, rows, 2 * width), BF),
            pltpu.VMEM((2, 2, 2, piece, width), BF),
            pltpu.VMEM((2, nz, 2, rows // 2, 2 * width), BF),
            pltpu.VMEM((nz, 2, piece, width), BF),
            pltpu.VMEM((2, queries, width), BF),
            pltpu.VMEM((2, 8, 128), F32),
            pltpu.VMEM((nz, 2, piece, value_width), BF),
            pltpu.VMEM((2 * nz, piece, value_width), BF),
            pltpu.VMEM((2, nz, PIECES, 2, depth // (2 * PIECES), units), BF),
            pltpu.VMEM((2, nz, PIECES, 2, units // 2, depth // PIECES), BF),
            pltpu.VMEM((nt,) + out_weight.shape, BF),
            pltpu.VMEM((4, piece, model), BF),
            pltpu.VMEM((rows, units), BF),
            pltpu.VMEM((n * PIECES, 4, piece, depth // PIECES), F32),
            pltpu.VMEM((n * PIECES, 4, piece, depth // PIECES), BF),
            pltpu.VMEM((n * PIECES, 2, piece, depth // PIECES), BF),
            pltpu.VMEM((n * PIECES, piece, depth // PIECES), BF),
            pltpu.VMEM((n * PIECES, piece, depth // PIECES), BF),
            pltpu.VMEM((2, tiles, 1, queries // tiles), F32),
            pltpu.VMEM((2, tiles, 1, queries // tiles), F32),
            pltpu.VMEM((2, tiles, value_width, queries // tiles), F32),
            pltpu.SemaphoreType.DMA((400,)),
            pltpu.SemaphoreType.DMA((slots,)),
            pltpu.SemaphoreType.DMA((8,)),
        ] + [pltpu.VMEM((rows, width), BF)] * 4,
        compiler_params=pltpu.CompilerParams(
            collective_id=0, has_side_effects=True, vmem_limit_bytes=60 * 2**20
        ),
        name="layer",
    )(first_query, second_query, first_key, second_key, values, inverse,
      lambdas, head_gain.reshape(1, -1), out_weight, residual,
      norm_gain.reshape(1, -1), up_weight, down_weight)


def choose(*args):
    n, nt = lax.axis_size("sp"), lax.axis_size("tp")
    residual, query, values, lambdas, out_weight, up_weight = (
        args[0], args[1], args[5], args[6], args[8], args[10]
    )
    rows, width = query.shape
    heads = lambdas.shape[0]
    fits = 2 * n * 2 * up_weight.size * 2 // 2 + nt * out_weight.size * 2 <= VMEM_BUDGET
    square = nt == 4 and n == 2 * nt and heads == 2 and width == 128
    square = square and values.shape[1] == 2 * width and rows == nt * residual.shape[0]
    if square and fits and up_weight.shape[0] == rows:
        return fused(n, nt, *args)
    return local(*args)


def solution(mesh):
    in_specs = (
        P(("sp", "tp"), None),
        P("sp", "tp"),
        P("sp", "tp"),
        P("sp", "tp"),
        P("sp", "tp"),
        P("sp", "tp"),
        P("tp"),
        P(),
        P("tp", None),
        P(),
        P("sp", "tp"),
        P("tp", "sp"),
    )
    out_specs = P(("sp", "tp"), None)
    return jax.shard_map(choose, mesh=mesh, in_specs=in_specs, out_specs=out_specs, check_vma=False)
```

```python
import functools

import jax
import jax.numpy as jnp
import numpy as np
from jax import lax
from jax.experimental import pallas as pl
from jax.experimental.pallas import tpu as pltpu
from jax.sharding import PartitionSpec as P


def rotate(blocked, positions):
    half = blocked.shape[-1] // 2
    inverse = 10000.0 ** (-jnp.arange(0, half, dtype=jnp.float32) * 2.0 / blocked.shape[-1])
    angle = positions[:, None] * inverse[None, :]
    cosine = jnp.cos(angle)[:, None, :]
    sine = jnp.sin(angle)[:, None, :]
    first, second = (blocked[..., :half], blocked[..., half:])
    return jnp.concatenate(
        [first * cosine - second * sine, second * cosine + first * sine], axis=-1
    )


def absorb(state, queries, keys, vals, factor):
    top, total, summed = state
    scores = jnp.einsum("qhe,khe->qhk", queries, keys, preferred_element_type=jnp.float32) * factor
    peak = jnp.maximum(top, jnp.max(scores, axis=-1))
    shrink = jnp.exp(top - peak)
    weights = jnp.exp(scores - peak[..., None])
    total = total * shrink + jnp.sum(weights, axis=-1)
    summed = summed * shrink[..., None] + jnp.einsum(
        "qhk,khe->qhe", weights.astype(jnp.bfloat16), vals, preferred_element_type=jnp.float32
    )
    return (peak, total, summed)


def layer_norm(stream, gain):
    center = stream - jnp.mean(stream, axis=-1, keepdims=True)
    spread = jnp.mean(center * center, axis=-1, keepdims=True)
    return center * lax.rsqrt(spread + 1e-05) * gain


def local(
    residual,
    first_query,
    second_query,
    first_key,
    second_key,
    values,
    lambdas,
    head_gain,
    out_weight,
    norm_gain,
    up_weight,
    down_weight,
):
    local_rows = first_query.shape[0]
    head_count = lambdas.shape[0]
    head_width = first_query.shape[1] // head_count
    value_width = values.shape[1] // head_count
    quarter_rows = local_rows // lax.axis_size("tp")
    factor = head_width ** (-0.5)
    positions = (lax.axis_index("sp") * local_rows + jnp.arange(local_rows)).astype(jnp.float32)

    def prepare(source):
        turned = rotate(
            source.astype(jnp.float32).reshape(local_rows, head_count, head_width), positions
        )
        return turned.astype(jnp.bfloat16)

    query_a, query_b = (prepare(first_query), prepare(second_query))
    key_a = prepare(first_key).reshape(local_rows, head_count * head_width)
    key_b = prepare(second_key).reshape(local_rows, head_count * head_width)
    start_state = (
        jnp.full((local_rows, head_count), -1e30, jnp.float32),
        jnp.zeros((local_rows, head_count), jnp.float32),
        jnp.zeros((local_rows, head_count, value_width), jnp.float32),
    )
    piece_a = lax.all_gather(key_a, "sp", axis=0, tiled=True)
    piece_b = lax.all_gather(key_b, "sp", axis=0, tiled=True)
    piece_v = lax.all_gather(values, "sp", axis=0, tiled=True)
    count = piece_a.shape[0]
    block = 512
    blocks = count // block

    def advance(state, item):
        block_a, block_b, block_v = item
        return (
            (
                absorb(state[0], query_a, block_a, block_v, factor),
                absorb(state[1], query_b, block_b, block_v, factor),
            ),
            None,
        )

    items = (
        piece_a.reshape(blocks, block, head_count, head_width),
        piece_b.reshape(blocks, block, head_count, head_width),
        piece_v.reshape(blocks, block, head_count, value_width),
    )
    state_a, state_b = lax.scan(advance, (start_state, start_state), items)[0]
    diff = state_a[2] / state_a[1][..., None] - lambdas[None, :, None] * (
        state_b[2] / state_b[1][..., None]
    )
    scale = lax.rsqrt(jnp.mean(diff * diff, axis=-1, keepdims=True) + 1e-05)
    flat = (
        (diff * scale * head_gain * 0.8)
        .astype(jnp.bfloat16)
        .reshape(local_rows, head_count * value_width)
    )
    projected = lax.psum(
        jnp.dot(flat, out_weight, preferred_element_type=jnp.float32).astype(jnp.bfloat16), "tp"
    ).astype(jnp.float32)
    stream = lax.all_gather(residual, "tp", axis=0, tiled=True)
    whole = layer_norm(stream.astype(jnp.float32) + projected, norm_gain).astype(jnp.bfloat16)
    own_normed = lax.dynamic_slice_in_dim(
        whole, lax.axis_index("tp") * quarter_rows, quarter_rows, 0
    )
    lifted = jnp.dot(
        whole,
        lax.all_gather(up_weight, "sp", axis=0, tiled=True),
        preferred_element_type=jnp.float32,
    )
    down_full = lax.all_gather(down_weight, "sp", axis=1, tiled=True)
    hidden = jnp.square(jax.nn.relu(lifted)).astype(jnp.bfloat16)
    lowered = lax.psum_scatter(
        jnp.dot(hidden, down_full, preferred_element_type=jnp.float32).astype(jnp.bfloat16),
        "tp",
        scatter_dimension=0,
        tiled=True,
    ).astype(jnp.float32)
    return (own_normed.astype(jnp.float32) + lowered).astype(jnp.bfloat16)


BF = jnp.bfloat16
F32 = jnp.float32
VMEM_BUDGET = 40 * 2**20
PIECES = 2
MESH = pl.DeviceIdType.MESH


def receive_slots(nz):
    sizes = dict(kvz=nz, kvx=nz, kvs=nz, kvt=nz, q=nz, head=2 * nz, lam=1, ow=6, norm=6)
    for name in ("up", "dn"):
        for way in "zxst":
            sizes[name + way] = nz * PIECES
    sizes.update(yg=2 * nz * PIECES, zg=2 * nz * PIECES)
    base, at = {}, 0
    for name, size in sizes.items():
        base[name] = at
        at += size
    return base, at


def layer_kernel(
    nz, head_width,
    qa_far, qb_far, ka_far, kb_far, v_far, inverse, lam, hgain, ow0, res0, ngain, up0, dn0,
    out,
    kvs, qs, kv, qb, qm, lamt, hsrc, hb, up, dn, ow, res, nb, hidden, mine, part, ygot, zsend, zgot,
    top, total, summed, send, recv, load, qa, qbb, ka, kb,
):
    s = lax.axis_index("sp")
    t = lax.axis_index("tp")
    z, x, y, c = s // 2, s % 2, t // 2, t % 2
    zl, zh = z % 2, z // 2
    pal = z + 1 - 2 * zl
    base, _ = receive_slots(nz)
    rows, width = ka.shape
    piece = res0.shape[0]
    depth = up0.shape[0]
    units = up0.shape[1]
    half_rows = rows // 2
    P_ = PIECES

    def dev(x_, y_, z_, c_):
        return {"sp": z_ * 2 + x_, "tp": y_ * 2 + c_}

    sib = dev(x, y, z, 1 - c)
    xnb = dev(1 - x, y, z, c)
    ynb = dev(x, 1 - y, z, c)
    znb = dev(x, y, pal, c)
    order = [z, pal, (z + 2) % nz, nz - 1 - z]

    loads = [
        pltpu.make_async_copy(src, dst, load.at[i])
        for i, (src, dst) in enumerate((
            (ka_far, ka), (kb_far, kb), (qa_far, qa), (qb_far, qbb),
            (v_far.at[:, :width], kvs.at[0, :, width:]), (v_far.at[:, width:], kvs.at[1, :, width:]),
            (ow0, ow.at[t]),
        ))
    ]
    for cp in loads:
        cp.start()
    barrier = pltpu.get_barrier_semaphore()
    peers = [xnb, sib]
    peers += [dev(x, y, (z + k) % nz, d) for k in range(1, nz) for d in range(2)]
    peers += [dev(x, 1 - y, (z + k) % nz, c) for k in range(nz)]
    for peer in peers:
        pl.semaphore_signal(barrier, inc=1, device_id=peer, device_id_type=MESH)

    started = []

    def remote(src, dst, slot, peer, unless=None):
        i = len(started)
        cp = pltpu.make_async_remote_copy(
            src_ref=src, dst_ref=dst, send_sem=send.at[i], recv_sem=recv.at[slot],
            device_id=peer, device_id_type=MESH,
        )
        started.append((cp, unless))
        if unless is None:
            cp.start()
        else:
            pl.when(jnp.logical_not(unless))(cp.start)

    def got(dst, slot, unless=None):
        cp = pltpu.make_async_remote_copy(
            src_ref=dst, dst_ref=dst, send_sem=send.at[0], recv_sem=recv.at[slot],
            device_id=sib, device_id_type=MESH,
        )
        if unless is None:
            cp.wait_recv()
        else:
            pl.when(jnp.logical_not(unless))(cp.wait_recv)

    def ow_half(ref, i):
        return ref.at[pl.ds(i * (rows // 2), rows // 2)]

    weights = {"up": (up0, up), "dn": (dn0, dn)}

    def spread(name, far, pieces=range(P_)):
        own, buf = weights[name]
        size = buf.shape[4]
        span = buf.shape[5]
        for p in pieces:
            for d in range(2):
                if name == "up":
                    src = own.at[pl.ds((d * P_ + p) * size, size)]
                else:
                    src = own.at[pl.ds(d * size, size), pl.ds(p * span, span)]
                dst = buf.at[x, z, p, d]
                slot = base[name + "z"] + z * P_ + p
                if far:
                    remote(src, dst, slot, dev(x, y, jnp.where(zl == c, (z + 2) % nz, 2 * (1 - zh) + c), d))
                    remote(src, dst, slot, dev(x, y, pal, d), unless=zl == c)
                else:
                    remote(src, dst, slot, sib, unless=jnp.logical_or(zl != c, d == c))
                    near = jnp.logical_and(zl == c, d == c)
                    pl.when(near)(pltpu.make_async_copy(src, dst, recv.at[slot]).start)

    def relay_z(name, k, pieces=range(P_)):
        buf = weights[name][1]
        zz = order[k]
        for p in pieces:
            ref = buf.at[x, zz, p, c]
            slot = base[name + "z"] + zz * P_ + p
            got(ref, slot)
            remote(ref, ref, base[name + "x"] + zz * P_ + p, xnb)
            remote(ref, ref, base[name + "s"] + zz * P_ + p, sib)

    def relay_x(name, k, pieces=range(P_)):
        buf = weights[name][1]
        zz = order[k]
        for p in pieces:
            ref = buf.at[1 - x, zz, p, c]
            got(ref, base[name + "x"] + zz * P_ + p)
            remote(ref, ref, base[name + "t"] + zz * P_ + p, sib)

    def settle(name, k, other, pieces=range(P_)):
        buf = weights[name][1]
        zz = order[k]
        for p in pieces:
            ref = buf.at[1 - x if other else x, zz, p, 1 - c]
            got(ref, base[name + ("t" if other else "s")] + zz * P_ + p)

    half = head_width // 2
    lane = lax.broadcasted_iota(jnp.int32, (rows, width), 1)
    low = (lane % head_width) < half
    front = lane < head_width
    position = (lax.broadcasted_iota(jnp.int32, (rows, width), 0) + s * rows).astype(F32)
    angle = position * inverse[...]
    cos = jnp.cos(angle)
    sin = jnp.sin(angle)
    sin = jnp.where(low, -sin, sin)

    def turn(ref):
        v = ref[...].astype(F32)
        other = jnp.where(low, pltpu.roll(v, width - half, 1), pltpu.roll(v, half, 1))
        return v * cos + other * sin

    def packed(a, b):
        first = jnp.where(front, a, pltpu.roll(b, head_width, 1))
        second = jnp.where(front, pltpu.roll(a, head_width, 1), b)
        return first.astype(BF), second.astype(BF)

    lamt[0] = jnp.full(lamt.shape[1:], lam[zl], F32)
    for cp in loads[:2]:
        cp.wait()
    for j, v in enumerate(packed(turn(ka), turn(kb))):
        kvs[j, :, :width] = v
    for cp in loads[2:4]:
        cp.wait()
    scale = head_width ** (-0.5)
    for j, v in enumerate(packed(turn(qa), turn(qbb))):
        qs[j] = (v.astype(F32) * scale).astype(BF).reshape(qs.shape[1:])
    for cp in loads[4:6]:
        cp.wait()
    pl.semaphore_wait(barrier, len(peers))
    for j in range(2):
        z_t = 2 * c + j
        for d in range(2):
            here = jnp.logical_and(z_t == z, d == c)
            peer = dev(x, y, z_t, d)
            src = kvs.at[j, pl.ds(d * half_rows, half_rows)]
            remote(src, kv.at[x, z, d], base["kvz"] + z, peer, unless=here)
    for j in range(2):
        z_t = 2 * c + j
        for d in range(2):
            here = jnp.logical_and(z_t == z, d == c)
            remote(qs.at[j, :, d], qb.at[zh, zl], base["q"] + z, dev(x, y, z_t, d), unless=here)
    spread("up", False)
    for i in range(2):
        remote(ow_half(ow0, i), ow_half(ow.at[t], i), base["ow"] + 2 + i, ynb)
    for i in range(2):
        remote(ow_half(ow0, i), ow_half(ow.at[t], i), base["ow"] + i, sib)
    remote(lamt.at[0], lamt.at[1], base["lam"], sib)
    mine_here = c == zh

    @pl.when(mine_here)
    def _():
        kv[x, z, c] = kvs[zl, pl.ds(pl.multiple_of(c * half_rows, half_rows), half_rows), :]
        for i in range(2):
            qb[zh, zl, i] = qs[zl, i, c]

    def relay_kv(k):
        zz = order[k]
        ref = kv.at[x, zz, c]
        got(ref, base["kvz"] + zz, mine_here if k == 0 else None)
        remote(ref, ref, base["kvx"] + zz, xnb)
        remote(ref, ref, base["kvs"] + zz, sib)

    def take_queries():
        for k in range(nz):
            zz = order[k]
            got(qb.at[zz // 2, zz % 2], base["q"] + zz, mine_here if k == 0 else None)
        queries = qb[...].reshape(-1, width)
        first_lanes = lax.broadcasted_iota(jnp.int32, queries.shape, 1) < head_width
        zero = jnp.zeros_like(queries)
        qm[0] = jnp.where(first_lanes, queries, zero)
        qm[1] = jnp.where(first_lanes, zero, queries)

    tiles = top.shape[1]
    tile = qm.shape[1] // tiles

    def attend(xi, first):
        def body(qt, carry):
            block = kv[xi].reshape(-1, 2 * width)
            keys = block[:, :width]
            vals = block[:, width:]
            at = pl.ds(pl.multiple_of(qt * tile, tile), tile)
            for m in range(2):
                scores = lax.dot_general(
                    keys, qm[m, at, :], (((1,), (1,)), ((), ())), preferred_element_type=F32
                )
                peak = jnp.max(scores, axis=0, keepdims=True)
                if not first:
                    old = top[m, qt]
                    peak = jnp.maximum(old, peak)
                    shrink = jnp.exp(old - peak)
                e = jnp.exp(scores - peak)
                row = jnp.sum(e, axis=0, keepdims=True)
                acc = lax.dot_general(
                    vals, e.astype(BF), (((0,), (0,)), ((), ())), preferred_element_type=F32
                )
                if first:
                    top[m, qt] = peak
                else:
                    row += total[m, qt] * shrink
                    acc += summed[m, qt] * shrink
                total[m, qt] = row
                summed[m, qt] = acc
            return carry

        lax.fori_loop(0, tiles, body, 0)

    def near_keys():
        for k in range(nz):
            got(kv.at[x, order[k], 1 - c], base["kvs"] + order[k])

    def relay_keys(k):
        ref = kv.at[1 - x, order[k], c]
        got(ref, base["kvx"] + order[k])
        remote(ref, ref, base["kvt"] + order[k], sib)

    def far_keys():
        for k in range(nz):
            got(kv.at[1 - x, order[k], 1 - c], base["kvt"] + order[k])

    there = 2 * (1 - y) + c
    me = y * nz + z

    def finish_heads():
        got(lamt.at[1], base["lam"])
        weight = jnp.where(mine_here, lamt[0], lamt[1])[:1, :1]
        for qt in range(tiles):
            a = summed[0, qt] / total[0, qt]
            b = summed[1, qt] / total[1, qt]
            diff = a - weight * b
            norm = lax.rsqrt(jnp.mean(diff * diff, axis=0, keepdims=True) + 1e-05)
            hsrc[qt] = ((diff * norm).T * hgain[...] * 0.8).astype(BF)
            for z_t in range(2 * qt, 2 * qt + 2):
                remote(
                    hsrc.at[qt], hb.at[me], base["head"] + me, dev(x, y, z_t, c), unless=z == z_t,
                )
        hb[me] = hsrc[zh]
        remote(hb.at[me], hb.at[me], base["head"] + me, ynb)

    def relay_heads(k):
        at = y * nz + order[k]
        got(hb.at[at], base["head"] + at)
        remote(hb.at[at], hb.at[at], base["head"] + at, ynb)

    def far_heads():
        for k in range(nz):
            at = (1 - y) * nz + order[k]
            got(hb.at[at], base["head"] + at)

    def relay_ow(i):
        ref = ow_half(ow.at[there], i)
        got(ref, base["ow"] + 2 + i)
        remote(ref, ref, base["ow"] + 4 + i, sib)

    own = 2 * zl + y
    zn = 2 * (1 - zl) + y

    def res_z():
        remote(res0, res.at[own], base["norm"], znb)

    def res_y():
        remote(res0, res.at[own], base["norm"] + 1, ynb)

    def relay_res():
        got(res.at[zn], base["norm"])
        remote(res.at[zn], res.at[zn], base["norm"] + 2, ynb)

    def project():
        loads[6].wait()
        for i in range(2):
            got(ow_half(ow.at[t + 1 - 2 * c], i), base["ow"] + i)
            got(ow_half(ow.at[there + 1 - 2 * c], i), base["ow"] + 4 + i)
        got(res.at[2 * zl + 1 - y], base["norm"] + 1)
        got(res.at[2 * (1 - zl) + 1 - y], base["norm"] + 2)
        res[own] = res0[...]

        def body(i, carry):
            at = pl.ds(pl.multiple_of(i * 2 * piece, 2 * piece), 2 * piece)
            stream = res[pl.ds(2 * i, 2)].reshape(2 * piece, -1).astype(F32)
            for tt in range(ow.shape[0]):
                pair = jnp.concatenate([hb[2 * tt, at, :], hb[2 * tt + 1, at, :]], axis=-1)
                stream += jnp.dot(pair, ow[tt], preferred_element_type=F32)
            center = stream - jnp.mean(stream, axis=-1, keepdims=True)
            spread_ = jnp.mean(center * center, axis=-1, keepdims=True)
            row = (center * lax.rsqrt(spread_ + 1e-05) * ngain[...]).astype(BF)
            nb[pl.ds(2 * i, 2)] = row.reshape(2, piece, -1)
            return carry

        lax.fori_loop(0, 2, body, 0)

    def lift():
        for k in range(nz):
            settle("up", k, False)
            settle("up", k, True)
        normed = nb[...].reshape(-1, nb.shape[2])
        lifted = None
        for zz in range(nz):
            for xx in range(2):
                at = (2 * zz + xx) * depth
                block = jnp.concatenate(
                    [up[xx, zz, p, d] for d in range(2) for p in range(P_)], axis=0
                )
                term = jnp.dot(normed[:, at : at + depth], block, preferred_element_type=F32)
                lifted = term if lifted is None else lifted + term
        lifted = jnp.maximum(lifted, 0.0)
        hidden[...] = (lifted * lifted).astype(BF)

    def lower(k, other, p):
        zz, xx = order[k], (1 - x if other else x)
        settle("dn", k, other, [p])
        i = (2 * zz + xx) * P_ + p
        r = jnp.dot(hidden[...], dn[xx, zz, p].reshape(units, -1), preferred_element_type=F32)
        mine[i] = r.reshape(mine.shape[1:])
        part[i] = r.astype(BF).reshape(part.shape[1:])
        remote(part.at[i, :, 1 - y], ygot.at[i], base["yg"] + i, ynb)
        return i

    def middle(i):
        got(ygot.at[i], base["yg"] + i)
        zsend[i] = (mine[i, zn] + ygot[i, 1 - zl].astype(F32)).astype(BF)
        remote(zsend.at[i], zgot.at[i], base["zg"] + i, znb)

    def finish(i):
        got(zgot.at[i], base["zg"] + i)
        span = mine.shape[3]
        at = pl.ds(pl.multiple_of(i * span, span), span)
        r = nb[own, :, at].astype(F32) + mine[i, own] + ygot[i, zl].astype(F32) + zgot[i].astype(F32)
        out[:, at] = r.astype(BF)

    done = []
    passed = []

    def low(k, other, p):
        done.append(lower(k, other, p))

    def mid():
        i = done[len(passed)]
        passed.append(i)
        middle(i)

    res_y()
    relay_z("up", 0, [0])
    relay_z("up", 0, [1])
    res_z()
    relay_kv(0)
    relay_kv(1)
    relay_kv(2)
    relay_kv(3)
    spread("up", True, [0])
    spread("dn", False)
    take_queries()
    near_keys()
    relay_z("dn", 0, [0])
    relay_z("dn", 0, [1])
    attend(x, True)
    relay_keys(0)
    relay_keys(1)
    relay_keys(2)
    relay_keys(3)
    relay_x("up", 0, [0])
    relay_x("up", 0, [1])
    spread("up", True, [1])
    far_keys()
    attend(1 - x, False)
    relay_res()
    finish_heads()
    relay_z("up", 1, [0])
    relay_z("up", 2, [0])
    relay_z("up", 3, [0])
    relay_ow(0)
    relay_heads(1)
    relay_heads(2)
    relay_heads(3)
    relay_ow(1)
    spread("dn", True, [0])
    relay_x("up", 1, [0])
    relay_x("up", 2, [0])
    relay_x("up", 3, [0])
    relay_z("up", 1, [1])
    relay_z("up", 2, [1])
    relay_z("up", 3, [1])
    spread("dn", True, [1])
    far_heads()
    project()
    relay_x("dn", 0, [0])
    relay_x("dn", 0, [1])
    relay_x("up", 1, [1])
    relay_x("up", 2, [1])
    relay_x("up", 3, [1])
    relay_z("dn", 1, [0])
    relay_z("dn", 2, [0])
    relay_z("dn", 3, [0])
    lift()
    low(0, False, 0)
    low(0, True, 0)
    relay_x("dn", 1, [0])
    relay_x("dn", 2, [0])
    relay_x("dn", 3, [0])
    low(1, False, 0)
    mid()
    low(1, True, 0)
    mid()
    relay_z("dn", 1, [1])
    low(2, False, 0)
    mid()
    low(2, True, 0)
    mid()
    relay_z("dn", 2, [1])
    low(3, False, 0)
    mid()
    low(3, True, 0)
    mid()
    relay_z("dn", 3, [1])
    low(0, False, 1)
    mid()
    low(0, True, 1)
    mid()
    relay_x("dn", 1, [1])
    low(1, False, 1)
    mid()
    low(1, True, 1)
    mid()
    relay_x("dn", 2, [1])
    low(2, False, 1)
    mid()
    low(2, True, 1)
    mid()
    relay_x("dn", 3, [1])
    low(3, False, 1)
    mid()
    low(3, True, 1)
    mid()
    mid()
    mid()
    for i in done:
        finish(i)
    for cp, unless in started:
        if unless is None:
            cp.wait_send()
        else:
            pl.when(jnp.logical_not(unless))(cp.wait_send)


def fused(n, nt, residual, first_query, second_query, first_key, second_key, values,
          lambdas, head_gain, out_weight, norm_gain, up_weight, down_weight):
    rows, width = first_query.shape
    heads = lambdas.shape[0]
    head_width = width // heads
    value_width = values.shape[1] // heads
    half = head_width // 2
    depth, units = up_weight.shape
    model = out_weight.shape[1]
    piece = residual.shape[0]
    nz = n // 2
    inverse = 10000.0 ** (-np.arange(half) * 2.0 / head_width)
    inverse = np.tile(inverse, 2 * heads)[None, :].astype(np.float32)
    vmem = pl.BlockSpec(memory_space=pltpu.VMEM)
    smem = pl.BlockSpec(memory_space=pltpu.SMEM)
    far = pl.BlockSpec(memory_space=pl.ANY)
    queries = rows * 2
    tiles = 2
    _, slots = receive_slots(nz)
    return pl.pallas_call(
        functools.partial(layer_kernel, nz, head_width),
        out_shape=jax.ShapeDtypeStruct((piece, model), BF),
        in_specs=[far] * 5 + [vmem, smem, vmem, far, vmem, vmem, far, far],
        out_specs=vmem,
        scratch_shapes=[
            pltpu.VMEM((2, rows, 2 * width), BF),
            pltpu.VMEM((2, 2, 2, piece, width), BF),
            pltpu.VMEM((2, nz, 2, rows // 2, 2 * width), BF),
            pltpu.VMEM((2, nz // 2, 2, piece, width), BF),
            pltpu.VMEM((2, queries, width), BF),
            pltpu.VMEM((2, 8, 128), F32),
            pltpu.VMEM((2, rows, value_width), BF),
            pltpu.VMEM((2 * nz, rows, value_width), BF),
            pltpu.VMEM((2, nz, PIECES, 2, depth // (2 * PIECES), units), BF),
            pltpu.VMEM((2, nz, PIECES, 2, units // 2, depth // PIECES), BF),
            pltpu.VMEM((nt,) + out_weight.shape, BF),
            pltpu.VMEM((4, piece, model), BF),
            pltpu.VMEM((4, piece, model), BF),
            pltpu.VMEM((rows, units), BF),
            pltpu.VMEM((n * PIECES, 4, piece, depth // PIECES), F32),
            pltpu.VMEM((n * PIECES, 2, 2, piece, depth // PIECES), BF),
            pltpu.VMEM((n * PIECES, 2, piece, depth // PIECES), BF),
            pltpu.VMEM((n * PIECES, piece, depth // PIECES), BF),
            pltpu.VMEM((n * PIECES, piece, depth // PIECES), BF),
            pltpu.VMEM((2, tiles, 1, queries // tiles), F32),
            pltpu.VMEM((2, tiles, 1, queries // tiles), F32),
            pltpu.VMEM((2, tiles, value_width, queries // tiles), F32),
            pltpu.SemaphoreType.DMA((400,)),
            pltpu.SemaphoreType.DMA((slots,)),
            pltpu.SemaphoreType.DMA((8,)),
        ] + [pltpu.VMEM((rows, width), BF)] * 4,
        compiler_params=pltpu.CompilerParams(
            collective_id=0, has_side_effects=True, vmem_limit_bytes=60 * 2**20
        ),
        name="layer",
    )(first_query, second_query, first_key, second_key, values, inverse,
      lambdas, head_gain.reshape(1, -1), out_weight, residual,
      norm_gain.reshape(1, -1), up_weight, down_weight)


def choose(*args):
    n, nt = lax.axis_size("sp"), lax.axis_size("tp")
    residual, query, values, lambdas, out_weight, up_weight = (
        args[0], args[1], args[5], args[6], args[8], args[10]
    )
    rows, width = query.shape
    heads = lambdas.shape[0]
    fits = 2 * n * 2 * up_weight.size * 2 // 2 + nt * out_weight.size * 2 <= VMEM_BUDGET
    square = nt == 4 and n == 2 * nt and heads == 2 and width == 128
    square = square and values.shape[1] == 2 * width and rows == nt * residual.shape[0]
    if square and fits and up_weight.shape[0] == rows:
        return fused(n, nt, *args)
    return local(*args)


def solution(mesh):
    in_specs = (
        P(("sp", "tp"), None),
        P("sp", "tp"),
        P("sp", "tp"),
        P("sp", "tp"),
        P("sp", "tp"),
        P("sp", "tp"),
        P("tp"),
        P(),
        P("tp", None),
        P(),
        P("sp", "tp"),
        P("tp", "sp"),
    )
    out_specs = P(("sp", "tp"), None)
    return jax.shard_map(choose, mesh=mesh, in_specs=in_specs, out_specs=out_specs, check_vma=False)
```
